32 devices in a mesh: grp: 2 (over x), ep: 16 (over z, y, core).
Axes of the slice: x: 2, y: 2, z: 4, core: 2. Of those that a mesh axis runs over, the one named last changes fastest.
Arguments:
- hidden_in: bfloat16 [512, 2048], P(('grp', 'ep')), parts along dimension 0, may hold values from -6 to 6
- state_in: float32 [512, 64, 1024], P(('grp', 'ep')), parts along dimension 0, may hold values from -3 to 3
- norm_gain: float32 [2048], replicated, may hold values from 0.1 to 1.9
- w_recept: bfloat16 [2048, 1024], P(None, 'ep'), may hold values from -0.125 to 0.125
- w_key: bfloat16 [2048, 1024], P(None, 'ep'), may hold values from -0.125 to 0.125
- w_value: bfloat16 [2048, 1024], P(None, 'ep'), may hold values from -0.125 to 0.125
- decay_base: float32 [1024], replicated, may hold values from -4 to 2
- w_decay_down: bfloat16 [2048, 128], replicated, may hold values from -0.125 to 0.125
- w_decay_up: bfloat16 [128, 1024], replicated, may hold values from -0.5 to 0.5
- w_remove_down: bfloat16 [2048, 128], replicated, may hold values from -0.125 to 0.125
- w_remove_up: bfloat16 [128, 1024], replicated, may hold values from -1 to 1
- group_gain: float32 [1024], replicated, may hold values from 0.1 to 1.9
- w_out: bfloat16 [1024, 2048], replicated, may hold values from -0.1875 to 0.1875
- ffn_gain: float32 [2048], replicated, may hold values from 0.1 to 1.9
- routes: int32 [512, 2], P(('grp', 'ep')), parts along dimension 0, may hold values from 0 to 3, all different within a row; in each aligned block of 16 rows (0 to 15, 16 to 31, ...) at most 16 rows name the same one
- route_gate: float32 [512, 2], P(('grp', 'ep')), parts along dimension 0, may hold values from 0.1 to 1
- w_gate: bfloat16 [2048, 11264], P(None, 'ep'), may hold values from -0.125 to 0.125
- w_up: bfloat16 [2048, 11264], P(None, 'ep'), may hold values from -0.125 to 0.125
- w_down: bfloat16 [11264, 2048], P('ep'), may hold values from -0.109375 to 0.109375
Outputs:
- mixed_out: bfloat16 [512, 2048], P(('grp', 'ep')), parts along dimension 0
- state_out: float32 [512, 64, 1024], P(('grp', 'ep')), parts along dimension 0
The draws below stay inside these ranges and needn't reach their ends.
There are 2 independent parts, one for each index of `grp`. The reference program is written for one: setup_inputs(seed, part) draws one part's arguments, and reference() takes and returns one part's arrays. A program takes and returns all parts, laid end to end along the dimension named above; an argument that names none is the same for every part. Nothing has to cross between parts.
Inputs may be any that keep to these rules, and one draw needn't show every extreme that they name: `routes`: each row names 2 different experts; in each aligned block of 16 rows (the rows of one device) no expert is named more than 16 times.
All inputs are finite; a program needn't handle non-finite values.
Results may differ from the reference program's by a relative error of at most 0.015.
Values may be sent and summed in bfloat16 or wider, within the bound.
No kernel may reach another device: no remote copies, remote signals or barrier semaphores. Data moves between devices by JAX's collectives and lax.ppermute only.
A program may use at most 128 MiB of HBM per device.

```python
import math
import jax
import jax.numpy as jnp
import numpy as np
from jax import lax

D = 2048
HS = 64
RANK = 128
EXP_FF = 2816
EXP_SPLIT = 4
TOPK = 2
S_DEV = 16
INNER = 1024
SEQS = 256
EXPERTS = 4
CAP = 16
N_EP = 16


def steps_of(stream_key, extent, shards, smallest, high):
    def one(axis_at, shards_of):
        draws = jax.random.uniform(jax.random.fold_in(jax.random.fold_in(stream_key, 6), axis_at), (shards_of,), jnp.float32, smallest / len(shards), high / len(shards))
        return jnp.repeat(jnp.exp(draws), extent[axis_at] // shards_of).reshape((-1,) + (1,) * (len(extent) - axis_at - 1))

    level = one(*shards[0])
    for cut in shards[1:]:
        level = level * one(*cut)
    return level


def deal_out(rng, own, number, rows, number_of, top, most, lean):
    sequence = jax.random.permutation(rng, number_of)
    heavy_load, ordinary = shares(number_of, rows * top, most, lean, True), shares(number_of, rows * top, most, lean, False)
    places = jnp.arange(number_of)

    def named(sizes, rotation):
        used = int((sizes > 0).sum())
        fixed = max(1, used // 4)
        passed = fixed + (places - fixed + rotation * (used - fixed)) % max(1, number_of - fixed)
        return jnp.zeros((number_of,), jnp.int32).at[sequence[jnp.where(places < fixed, places, passed)]].set(jnp.asarray(sizes, jnp.int32))

    sizes = jnp.where(number % 4 == 0, named(heavy_load, number // 4), named(ordinary, number - number // 4 - 1))
    mixed = jax.random.permutation(jax.random.fold_in(own, 3), number_of)
    source_of, sink = mixed[0:number_of // 2 * 2:2], mixed[1:number_of // 2 * 2:2]
    margin = jnp.minimum(sizes[source_of] - 1, most - sizes[sink]) // 2
    margin = jnp.where((source_of == sequence[0]) | (sink == sequence[0]) | (sizes[sink] == 0), 0, jnp.maximum(margin, 0))
    passed = jax.random.randint(jax.random.fold_in(own, 4), (number_of // 2,), 0, 1 << 20) % (margin + 1)
    sizes = sizes.at[source_of].add(-passed).at[sink].add(passed)
    members = jnp.searchsorted(jnp.cumsum(sizes), jnp.arange(rows * top), side="right").astype(jnp.int32)
    listing = members.reshape(top, rows).T
    listing = listing[jax.random.permutation(jax.random.fold_in(own, 1), rows)]
    rotation = jax.random.randint(jax.random.fold_in(own, 2), (rows, 1), 0, top)
    return jnp.take_along_axis(listing, (jnp.arange(top)[None, :] + rotation) % top, axis=1)


def shares(number_of, total, limit, slope, full):
    portions = [(1 << 20) // math.isqrt(standing ** slope) + 1 for standing in range(1, number_of + 1)]
    largest = limit if full else min(limit, max(-(-total // number_of), total * portions[0] // sum(portions)))
    least = 1 if total - largest >= number_of - 1 else 0
    holding, surplus = [largest] + [least] * (number_of - 1), total - largest - least * (number_of - 1)
    while surplus > 0:
        free = [i for i in range(1, number_of) if holding[i] < largest] or [i for i in range(1, number_of) if holding[i] < limit]
        whole, left = sum([portions[i] for i in free]), surplus
        for i in free:
            extra = min(limit - holding[i], max(1, left * portions[i] // whole), surplus)
            holding[i] = holding[i] + extra
            surplus = surplus - extra
    return np.array(holding)


def bell_draw(key, extent, scale, most, cuts=(), kind=jnp.bfloat16):
    gain = steps_of(key, extent, cuts, -0.22, 0.18) if cuts else 1.0
    entries = jax.random.normal(key, extent, jnp.float32) * scale * gain
    return jnp.minimum(jnp.maximum(entries, -most), most).astype(kind)


def setup_inputs(seed: int = 0, part: int = 0) -> dict:
    splits = jax.random.split(jax.random.key(seed), 20)
    own_keys = jax.random.split(jax.random.fold_in(splits[19], part), 20)
    hidden_in = bell_draw(own_keys[0], (SEQS, D), 1.0, 6.0, ((0, 16),))
    state_in = bell_draw(own_keys[1], (SEQS, HS, INNER), 0.5, 3.0, ((0, 16),), jnp.float32)
    norm_gain = jnp.clip(1.0 + 0.18 * jax.random.normal(splits[2], (D,), jnp.float32), 0.1, 1.9)
    w_recept = bell_draw(splits[3], (D, INNER), D ** -0.5, 0.125, ((1, 16),))
    w_key = bell_draw(splits[4], (D, INNER), D ** -0.5, 0.125, ((1, 16),))
    w_value = bell_draw(splits[5], (D, INNER), D ** -0.5, 0.125, ((1, 16),))
    decay_base = jnp.clip(jax.random.uniform(splits[6], (INNER,), jnp.float32, -4.0, 2.0), -4.0, 2.0)
    w_decay_down = bell_draw(splits[7], (D, RANK), D ** -0.5, 0.125)
    w_decay_up = bell_draw(splits[8], (RANK, INNER), RANK ** -0.5, 0.5)
    w_remove_down = bell_draw(splits[9], (D, RANK), D ** -0.5, 0.125)
    w_remove_up = bell_draw(splits[10], (RANK, INNER), (RANK // 4) ** -0.5, 1.0)
    group_gain = jnp.clip(1.0 + 0.18 * jax.random.normal(splits[11], (INNER,), jnp.float32), 0.1, 1.9)
    w_out = bell_draw(splits[12], (INNER, D), INNER ** -0.5, 0.1875)
    ffn_gain = jnp.clip(1.0 + 0.18 * jax.random.normal(splits[13], (D,), jnp.float32), 0.1, 1.9)
    routes_keys = jax.random.split(jax.random.fold_in(own_keys[14], 1), SEQS // S_DEV)
    routes_turns = jax.random.permutation(jax.random.fold_in(own_keys[14], 3), SEQS // S_DEV)
    routes = jax.vmap(lambda own, number: deal_out(jax.random.fold_in(own_keys[14], 2), own, number, S_DEV, EXPERTS, TOPK, CAP, 2))(routes_keys, routes_turns).reshape((SEQS, TOPK))
    route_gate = jnp.clip(0.1 + 0.9 * jax.random.uniform(own_keys[15], (SEQS, TOPK), jnp.float32) ** steps_of(own_keys[15], (SEQS, TOPK), ((0, 16),), -0.2, 0.2), 0.1, 1.0)
    w_gate = bell_draw(splits[16], (D, EXPERTS * EXP_FF), D ** -0.5, 0.125, ((1, 16),))
    w_up = bell_draw(splits[17], (D, EXPERTS * EXP_FF), D ** -0.5, 0.125, ((1, 16),))
    w_down = bell_draw(splits[18], (EXPERTS * EXP_FF, D), EXP_FF ** -0.5, 0.109375, ((0, 16),))
    return {"hidden_in": hidden_in, "state_in": state_in, "norm_gain": norm_gain, "w_recept": w_recept, "w_key": w_key, "w_value": w_value, "decay_base": decay_base, "w_decay_down": w_decay_down, "w_decay_up": w_decay_up, "w_remove_down": w_remove_down, "w_remove_up": w_remove_up, "group_gain": group_gain, "w_out": w_out, "ffn_gain": ffn_gain, "routes": routes, "route_gate": route_gate, "w_gate": w_gate, "w_up": w_up, "w_down": w_down}


norm_eps = 1e-06
group_eps = 0.00064

def scaled_rows(values, scale_gain):
    floats = values.astype(jnp.float32)
    return floats * lax.rsqrt(lax.optimization_barrier(jnp.mean(floats * floats, axis=-1, keepdims=True)) + norm_eps) * scale_gain

def update_state(state_in, receptance, new_keys, new_values, decay_rate, removal):
    seq_count = state_in.shape[0]
    head_size = state_in.shape[1]
    head_count = state_in.shape[2] // head_size
    shape_heads = (seq_count, head_count, head_size)
    recept_heads = receptance.astype(jnp.float32).reshape(shape_heads)
    key_heads = new_keys.astype(jnp.float32).reshape(shape_heads)
    value_heads = new_values.astype(jnp.float32).reshape(shape_heads)
    unit_keys = key_heads * lax.rsqrt(lax.optimization_barrier(jnp.sum(key_heads * key_heads, axis=-1, keepdims=True)) + norm_eps)
    blocks = state_in.reshape(seq_count, head_size, head_count, head_size)
    recalled = jnp.einsum('svhk,shk->svh', blocks, unit_keys, precision=lax.Precision.HIGHEST)
    removed = unit_keys * removal.reshape(shape_heads)
    updated = blocks * decay_rate.reshape(seq_count, 1, head_count, head_size) - recalled[..., None] * removed[:, None] + jnp.swapaxes(value_heads, 1, 2)[..., None] * key_heads[:, None]
    readout = jnp.einsum('svhk,shk->shv', updated, recept_heads, precision=lax.Precision.HIGHEST)
    return (updated.reshape(state_in.shape), readout)

def group_scale(readout, scale_gain):
    center = readout - lax.optimization_barrier(jnp.mean(readout, axis=-1, keepdims=True))
    spread = lax.optimization_barrier(jnp.mean(center * center, axis=-1, keepdims=True))
    normed = center * lax.rsqrt(spread + group_eps)
    return (normed.reshape(readout.shape[0], -1) * scale_gain).astype(jnp.bfloat16)

def decay_of(normed, w_decay_down, w_decay_up, decay_base):
    decay_low = jnp.dot(normed, w_decay_down, preferred_element_type=jnp.float32).astype(jnp.bfloat16)
    decay_act = jnp.tanh(decay_low.astype(jnp.float32)).astype(jnp.bfloat16)
    decay_pre = decay_base + jnp.dot(decay_act, w_decay_up, preferred_element_type=jnp.float32)
    return jnp.exp(-jnp.exp(-jax.nn.softplus(-decay_pre) - 0.5))

def removal_of(normed, w_remove_down, w_remove_up):
    remove_low = jnp.dot(normed, w_remove_down, preferred_element_type=jnp.float32).astype(jnp.bfloat16)
    return jax.nn.sigmoid(jnp.dot(remove_low, w_remove_up, preferred_element_type=jnp.float32))

def reference(hidden_in, state_in, norm_gain, w_recept, w_key, w_value, decay_base, w_decay_down, w_decay_up, w_remove_down, w_remove_up, group_gain, w_out, ffn_gain, routes, route_gate, w_gate, w_up, w_down):
    normed = scaled_rows(hidden_in, norm_gain).astype(jnp.bfloat16)
    receptance = jnp.dot(normed, w_recept, preferred_element_type=jnp.float32).astype(jnp.bfloat16)
    new_keys = jnp.dot(normed, w_key, preferred_element_type=jnp.float32).astype(jnp.bfloat16)
    new_values = jnp.dot(normed, w_value, preferred_element_type=jnp.float32).astype(jnp.bfloat16)
    decay_rate = decay_of(normed, w_decay_down, w_decay_up, decay_base)
    removal = removal_of(normed, w_remove_down, w_remove_up)
    state_out, readout = update_state(state_in, receptance, new_keys, new_values, decay_rate, removal)
    grouped = group_scale(readout, group_gain)
    residual = hidden_in.astype(jnp.float32) + jnp.dot(grouped, w_out, preferred_element_type=jnp.float32)
    expert_in = scaled_rows(residual, ffn_gain).astype(jnp.bfloat16)
    chosen = routes.reshape(N_EP, S_DEV * TOPK)
    hit_table = (chosen[..., None] == jnp.arange(EXPERTS, dtype=jnp.int32)).astype(jnp.int32)
    slot_index = lax.optimization_barrier(jnp.sum((jnp.cumsum(hit_table, axis=1) - 1) * hit_table, axis=2))
    slot_table = (slot_index[..., None] == jnp.arange(CAP, dtype=jnp.int32)).astype(jnp.float32)
    placed = hit_table.astype(jnp.float32)[..., None] * slot_table[:, :, None, :]
    placed = placed.reshape(N_EP, S_DEV, TOPK, EXPERTS, CAP)
    dispatch = lax.optimization_barrier(jnp.sum(placed, axis=2))
    combine = lax.optimization_barrier(jnp.sum(placed * route_gate.reshape(N_EP, S_DEV, TOPK)[..., None, None], axis=2))
    blocks_in = expert_in.reshape(N_EP, S_DEV, D).astype(jnp.float32)
    gathered = jnp.einsum('nsec,nsd->encd', dispatch, blocks_in, precision=lax.Precision.HIGHEST).astype(jnp.bfloat16)
    quarter = EXP_FF // EXP_SPLIT

    def run_expert(operands):
        inputs, index = operands
        flat_rows = inputs.reshape(N_EP * CAP, D)
        gate_cols = lax.dynamic_slice_in_dim(w_gate, index * EXP_FF, EXP_FF, 1)
        up_cols = lax.dynamic_slice_in_dim(w_up, index * EXP_FF, EXP_FF, 1)
        down_rows = lax.dynamic_slice_in_dim(w_down, index * EXP_FF, EXP_FF, 0)
        gate_pre = jnp.dot(flat_rows, gate_cols, preferred_element_type=jnp.float32)
        up_pre = jnp.dot(flat_rows, up_cols, preferred_element_type=jnp.float32)
        hidden = (jax.nn.silu(gate_pre) * up_pre).astype(jnp.bfloat16)
        parts = jnp.einsum('rqf,qfd->qrd', hidden.reshape(N_EP * CAP, EXP_SPLIT, quarter).astype(jnp.float32), down_rows.reshape(EXP_SPLIT, quarter, D).astype(jnp.float32))
        rounded = lax.optimization_barrier(parts.astype(jnp.bfloat16))
        return lax.optimization_barrier(jnp.sum(rounded.astype(jnp.float32), axis=0)).reshape(N_EP, CAP, D)
    outputs = lax.map(run_expert, (gathered, jnp.arange(EXPERTS, dtype=jnp.int32)))
    routed = jnp.einsum('nsec,encd->nsd', combine, outputs, precision=lax.Precision.HIGHEST).reshape(N_EP * S_DEV, D)
    mixed_out = (residual + routed).astype(jnp.bfloat16)
    return (mixed_out, state_out)
```

```python
import functools

import jax
import jax.numpy as jnp
from jax import lax
from jax.experimental import pallas as pl
from jax.experimental.pallas import tpu as pltpu
from jax.sharding import PartitionSpec as P

EXP_SPLIT = 4

norm_eps = 1e-06
group_eps = 0.00064
f32 = jnp.float32
bf16 = jnp.bfloat16
NT = (((1,), (1,)), ((), ()))
VM = pl.BlockSpec(memory_space=pltpu.VMEM)
ANY = pl.BlockSpec(memory_space=pl.ANY)


def scaled_rows(values, scale_gain):
    floats = values.astype(f32)
    return (
        floats
        * lax.rsqrt(jnp.mean(floats * floats, axis=-1, keepdims=True) + norm_eps)
        * scale_gain
    )


def decay_of(normed, w_decay_down, w_decay_up, decay_base):
    decay_low = jnp.dot(normed, w_decay_down, preferred_element_type=f32).astype(bf16)
    decay_act = jnp.tanh(decay_low.astype(f32)).astype(bf16)
    decay_pre = decay_base + jnp.dot(decay_act, w_decay_up, preferred_element_type=f32)
    return jnp.exp(-jnp.exp(-jax.nn.softplus(-decay_pre) - 0.5))


def removal_of(normed, w_remove_down, w_remove_up):
    remove_low = jnp.dot(normed, w_remove_down, preferred_element_type=f32).astype(bf16)
    return jax.nn.sigmoid(jnp.dot(remove_low, w_remove_up, preferred_element_type=f32))


def swap(piece, bits):
    size = lax.axis_size("ep")
    return lax.ppermute(piece, "ep", [(i, i ^ bits) for i in range(size)])


def gather_pieces(own):
    size = lax.axis_size("ep")
    pieces = {0: own}
    for d in range(size // 4 - 1, 0, -1):
        pieces[4 * d] = swap(own, 4 * d)
    for d in list(pieces):
        pieces[d + 2] = swap(pieces[d], 2)
    for d in list(pieces):
        pieces[d + 1] = swap(pieces[d], 1)
    return [pieces[d] for d in range(size)]


def norm_kernel(x_ref, gain_ref, out_ref):
    out_ref[...] = scaled_rows(x_ref[...], gain_ref[...]).astype(bf16)


def norm_rows(values, gain):
    return pl.pallas_call(
        norm_kernel,
        out_shape=jax.ShapeDtypeStruct(values.shape, bf16),
        in_specs=[VM, VM],
        out_specs=VM,
        name="norm_rows",
    )(values, gain.reshape(1, -1))


def project_kernel(place_ref, *refs):
    out_ref = refs[-1]
    count = out_ref.shape[0]
    pieces, weights = refs[:count], refs[count : count + 3]
    rows = pieces[0].shape[0]
    width = weights[0].shape[0]
    tokens = jnp.concatenate([piece[...] for piece in pieces], axis=0)
    parts = [
        lax.dot_general(tokens, w[...], NT, preferred_element_type=f32).astype(bf16)
        for w in weights
    ]
    place = place_ref[0]
    for d in range(count):
        target = place ^ d
        for m in range(3):
            out_ref[target, :, m * width : (m + 1) * width] = parts[m][d * rows : (d + 1) * rows]


def project(pieces, weights):
    count = len(pieces)
    rows = pieces[0].shape[0]
    width = weights[0].shape[1]
    return pl.pallas_call(
        project_kernel,
        out_shape=jax.ShapeDtypeStruct((count, rows, 3 * width), bf16),
        in_specs=[pl.BlockSpec(memory_space=pltpu.SMEM)] + [VM] * (count + 3),
        out_specs=VM,
        name="project",
    )(lax.axis_index("ep").astype(jnp.int32).reshape(1), *pieces, *[w.T for w in weights])


def mixer_kernel(
    state_ref, joined_ref, decay_ref, removal_ref, gain_ref, hidden_ref, ffn_gain_ref, w_out_ref,
    state_out_ref, residual_ref, expert_ref,
    vec_ref, readout_ref, w_out_buf, sem, *, head,
):
    step = pl.program_id(0)
    steps = pl.num_programs(0)
    batch, values, inner = state_ref.shape
    chunk = min(256, inner)
    count = joined_ref.shape[0]
    width = inner // count
    copy = pltpu.make_async_copy(w_out_ref, w_out_buf, sem)

    def ones(dtype, scale=1.0):
        a = lax.broadcasted_iota(jnp.int32, (chunk, chunk), 0) // head
        b = lax.broadcasted_iota(jnp.int32, (chunk, chunk), 1) // head
        return jnp.where(a == b, scale, 0.0).astype(dtype)

    def head_sums(x, block, precision=None):
        return jnp.concatenate(
            [
                jnp.dot(
                    x[:, c : c + chunk], block, preferred_element_type=f32, precision=precision
                )
                for c in range(0, inner, chunk)
            ],
            axis=1,
        )

    @pl.when(step == 0)
    def _():
        copy.start()
        for m in range(3):
            for j in range(count):
                vec_ref[m, :, j * width : (j + 1) * width] = joined_ref[
                    j, :, m * width : (m + 1) * width
                ].astype(f32)
        keys = vec_ref[1]
        unit = keys * lax.rsqrt(
            head_sums(keys * keys, ones(f32), lax.Precision.HIGHEST) + norm_eps
        )
        vec_ref[3] = unit
        vec_ref[4] = unit * removal_ref[...]

    block = ones(bf16)
    lane = lax.broadcasted_iota(jnp.int32, (values, inner), 1) % head
    row = lax.broadcasted_iota(jnp.int32, (values, inner), 0)
    diagonal = lane == row
    for b in range(batch):
        s = step * batch + b
        receptance = vec_ref[0, pl.ds(s, 1), :]
        keys = vec_ref[1, pl.ds(s, 1), :]
        new_values = vec_ref[2, pl.ds(s, 1), :]
        unit = vec_ref[3, pl.ds(s, 1), :]
        removed = vec_ref[4, pl.ds(s, 1), :]
        decay = decay_ref[pl.ds(s, 1), :]
        state = state_ref[b]
        recalled = head_sums((state * unit).astype(bf16), block)
        spread = head_sums(jnp.where(diagonal, new_values, 0.0).astype(bf16), block)
        updated = state * decay - recalled * removed + spread * keys
        state_out_ref[b] = updated
        read = head_sums((updated * receptance).astype(bf16), block)
        readout_ref[pl.ds(s, 1), :] = jnp.sum(
            jnp.where(diagonal, read, 0.0), axis=0, keepdims=True
        )

    @pl.when(step == steps - 1)
    def _():
        readout = readout_ref[...]
        mean_block = ones(f32, 1.0 / head)
        center = readout - head_sums(readout, mean_block, lax.Precision.HIGHEST)
        variance = head_sums(center * center, mean_block, lax.Precision.HIGHEST)
        grouped = (center * lax.rsqrt(variance + group_eps) * gain_ref[...]).astype(bf16)
        copy.wait()
        residual = hidden_ref[...].astype(f32) + jnp.dot(
            grouped, w_out_buf[...], preferred_element_type=f32
        )
        residual_ref[...] = residual
        expert_ref[...] = scaled_rows(residual, ffn_gain_ref[...]).astype(bf16)


def mixer(state_in, joined, decay, removal, group_gain, hidden_in, ffn_gain, w_out):
    seqs, head, inner = state_in.shape
    width = hidden_in.shape[1]
    batch = 4 if seqs % 4 == 0 else 1

    def whole(shape):
        return pl.BlockSpec(shape, lambda i: (0,) * len(shape))

    by_seq = pl.BlockSpec((batch, head, inner), lambda i: (i, 0, 0))
    return pl.pallas_call(
        functools.partial(mixer_kernel, head=head),
        grid=(seqs // batch,),
        out_shape=(
            jax.ShapeDtypeStruct(state_in.shape, f32),
            jax.ShapeDtypeStruct((seqs, width), f32),
            jax.ShapeDtypeStruct((seqs, width), bf16),
        ),
        in_specs=[
            by_seq,
            whole(joined.shape),
            whole((seqs, inner)),
            whole((seqs, inner)),
            whole((1, inner)),
            whole((seqs, width)),
            whole((1, width)),
            ANY,
        ],
        out_specs=(by_seq, whole((seqs, width)), whole((seqs, width))),
        scratch_shapes=[
            pltpu.VMEM((5, seqs, inner), f32),
            pltpu.VMEM((seqs, inner), f32),
            pltpu.VMEM(w_out.shape, bf16),
            pltpu.SemaphoreType.DMA(()),
        ],
        name="mixer",
    )(
        state_in, joined, decay, removal, group_gain.reshape(1, -1), hidden_in,
        ffn_gain.reshape(1, -1), w_out,
    )


def expert_kernel(*refs, count):
    pieces = refs[:count]
    gate_ref, up_ref, down_ref = refs[count : count + 3]
    outs = refs[count + 3 : -5]
    gate_buf, up_buf, down_buf, hidden_ref, sems = refs[-5:]
    rows = pieces[0].shape[0]
    units = gate_buf.shape[0]
    cuts = 2
    part = units // cuts
    copies = []
    for c in range(cuts):
        span = pl.ds(c * part, part)
        for m, (source, target) in enumerate(((gate_ref, gate_buf), (up_ref, up_buf))):
            copies.append(
                pltpu.make_async_copy(source.at[span], target.at[span], sems.at[2 * c + m])
            )
    last = pltpu.make_async_copy(down_ref, down_buf, sems.at[2 * cuts])
    for copy in copies:
        copy.start()
    last.start()
    tokens = jnp.concatenate([piece[...] for piece in pieces], axis=0)
    for c in range(cuts):
        span = pl.ds(c * part, part)
        copies[2 * c].wait()
        gate = lax.dot_general(tokens, gate_buf[span], NT, preferred_element_type=f32)
        copies[2 * c + 1].wait()
        up = lax.dot_general(tokens, up_buf[span], NT, preferred_element_type=f32)
        hidden_ref[:, c * part : (c + 1) * part] = (jax.nn.silu(gate) * up).astype(bf16)
    last.wait()
    result = jnp.dot(hidden_ref[...], down_buf[...], preferred_element_type=f32).astype(bf16)
    for d in range(count):
        outs[2 * (d // 4) + d % 2][d % 4 // 2] = result[d * rows : (d + 1) * rows]


def run_experts(pieces, w_gate, w_up, w_down):
    count = len(pieces)
    rows, width = pieces[0].shape
    units = w_down.shape[0]
    return pl.pallas_call(
        functools.partial(expert_kernel, count=count),
        out_shape=[jax.ShapeDtypeStruct((2, rows, width), bf16)] * (count // 2),
        in_specs=[VM] * count + [ANY] * 3,
        out_specs=[VM] * (count // 2),
        scratch_shapes=[pltpu.VMEM((units, width), bf16)] * 3
        + [pltpu.VMEM((count * rows, units), bf16), pltpu.SemaphoreType.DMA((5,))],
        name="experts",
    )(*pieces, w_gate.T, w_up.T, w_down)


def add(a, b):
    return (a.astype(f32) + b.astype(f32)).astype(bf16)


def shards(
    hidden_in,
    state_in,
    norm_gain,
    w_recept,
    w_key,
    w_value,
    decay_base,
    w_decay_down,
    w_decay_up,
    w_remove_down,
    w_remove_up,
    group_gain,
    w_out,
    ffn_gain,
    routes,
    route_gate,
    w_gate,
    w_up,
    w_down,
):
    place = lax.axis_index("ep")
    groups = lax.axis_size("ep") // EXP_SPLIT
    normed = norm_rows(hidden_in, norm_gain)
    pieces = gather_pieces(normed)
    spread = project(pieces, (w_recept, w_key, w_value))
    joined = lax.all_to_all(spread, "ep", split_axis=0, concat_axis=0, tiled=True)
    decay_rate = decay_of(normed, w_decay_down, w_decay_up, decay_base)
    removal = removal_of(normed, w_remove_down, w_remove_up)
    state_out, residual, expert_in = mixer(
        state_in, joined, decay_rate, removal, group_gain, hidden_in, ffn_gain, w_out
    )
    outs = run_experts(gather_pieces(expert_in), w_gate, w_up, w_down)
    mixed = residual
    for d in range(groups - 1, -1, -1):
        by_side = add(outs[2 * d], swap(outs[2 * d + 1], 1))
        part = add(by_side[0], swap(by_side[1], 2))
        if d:
            part = swap(part, EXP_SPLIT * d)
        weight = jnp.sum(
            jnp.where(routes == (place // EXP_SPLIT) ^ d, route_gate, 0.0), axis=1, keepdims=True
        )
        mixed = mixed + weight * part.astype(f32)
    return (mixed.astype(bf16), state_out)


def solution(mesh):
    placed = (
        P(("grp", "ep"), None),
        P(("grp", "ep"), None, None),
        P(),
        P(None, "ep"),
        P(None, "ep"),
        P(None, "ep"),
        P(),
        P(),
        P(),
        P(),
        P(),
        P(),
        P(),
        P(),
        P(("grp", "ep"), None),
        P(("grp", "ep"), None),
        P(None, "ep"),
        P(None, "ep"),
        P("ep", None),
    )
    return jax.shard_map(
        shards,
        mesh=mesh,
        in_specs=placed,
        out_specs=(P(("grp", "ep"), None), P(("grp", "ep"), None, None)),
        check_vma=False,
    )
```

```python
import functools

import jax
import jax.numpy as jnp
from jax import lax
from jax.experimental import pallas as pl
from jax.experimental.pallas import tpu as pltpu
from jax.sharding import PartitionSpec as P

EXP_SPLIT = 4

norm_eps = 1e-06
group_eps = 0.00064
f32 = jnp.float32
bf16 = jnp.bfloat16
NT = (((1,), (1,)), ((), ()))
VM = pl.BlockSpec(memory_space=pltpu.VMEM)
ANY = pl.BlockSpec(memory_space=pl.ANY)


def scaled_rows(values, scale_gain):
    floats = values.astype(f32)
    return (
        floats
        * lax.rsqrt(jnp.mean(floats * floats, axis=-1, keepdims=True) + norm_eps)
        * scale_gain
    )


def decay_of(normed, w_decay_down, w_decay_up, decay_base):
    decay_low = jnp.dot(normed, w_decay_down, preferred_element_type=f32).astype(bf16)
    decay_act = jnp.tanh(decay_low.astype(f32)).astype(bf16)
    decay_pre = decay_base + jnp.dot(decay_act, w_decay_up, preferred_element_type=f32)
    return jnp.exp(-jnp.exp(-jax.nn.softplus(-decay_pre) - 0.5))


def removal_of(normed, w_remove_down, w_remove_up):
    remove_low = jnp.dot(normed, w_remove_down, preferred_element_type=f32).astype(bf16)
    return jax.nn.sigmoid(jnp.dot(remove_low, w_remove_up, preferred_element_type=f32))


def swap(piece, bits):
    size = lax.axis_size("ep")
    return lax.ppermute(piece, "ep", [(i, i ^ bits) for i in range(size)])


def gather_pieces(own):
    size = lax.axis_size("ep")
    pieces = {0: own}
    for d in range(size // 4 - 1, 0, -1):
        pieces[4 * d] = swap(own, 4 * d)
    for d in list(pieces):
        pieces[d + 2] = swap(pieces[d], 2)
    for d in list(pieces):
        pieces[d + 1] = swap(pieces[d], 1)
    return [pieces[d] for d in range(size)]


def norm_kernel(x_ref, gain_ref, out_ref):
    out_ref[...] = scaled_rows(x_ref[...], gain_ref[...]).astype(bf16)


def norm_rows(values, gain):
    return pl.pallas_call(
        norm_kernel,
        out_shape=jax.ShapeDtypeStruct(values.shape, bf16),
        in_specs=[VM, VM],
        out_specs=VM,
        name="norm_rows",
    )(values, gain.reshape(1, -1))


def project_kernel(place_ref, *refs):
    out_ref = refs[-1]
    count = out_ref.shape[0]
    pieces, weights = refs[:count], refs[count : count + 3]
    rows = pieces[0].shape[0]
    width = weights[0].shape[0]
    gain = refs[count + 3][...]
    tokens = jnp.concatenate(
        [scaled_rows(piece[...], gain).astype(bf16) for piece in pieces], axis=0
    )
    parts = [
        lax.dot_general(tokens, w[...], NT, preferred_element_type=f32).astype(bf16)
        for w in weights
    ]
    place = place_ref[0]
    for d in range(count):
        target = place ^ d
        for m in range(3):
            out_ref[target, :, m * width : (m + 1) * width] = parts[m][d * rows : (d + 1) * rows]


def project(pieces, weights, gain):
    count = len(pieces)
    rows = pieces[0].shape[0]
    width = weights[0].shape[1]
    return pl.pallas_call(
        project_kernel,
        out_shape=jax.ShapeDtypeStruct((count, rows, 3 * width), bf16),
        in_specs=[pl.BlockSpec(memory_space=pltpu.SMEM)] + [VM] * (count + 4),
        out_specs=VM,
        compiler_params=pltpu.CompilerParams(vmem_limit_bytes=16 * 2**20),
        name="project",
    )(lax.axis_index("ep").astype(jnp.int32).reshape(1), *pieces, *[w.T for w in weights], gain.reshape(1, -1))


def mixer_kernel(
    state_ref, joined_ref, decay_ref, removal_ref, gain_ref, hidden_ref, ffn_gain_ref, w_out_ref,
    state_out_ref, residual_ref, expert_ref,
    vec_ref, readout_ref, w_out_buf, sem, *, head,
):
    step = pl.program_id(0)
    steps = pl.num_programs(0)
    batch, values, inner = state_ref.shape
    chunk = min(256, inner)
    count = joined_ref.shape[0]
    width = inner // count
    copy = pltpu.make_async_copy(w_out_ref, w_out_buf, sem)

    def ones(dtype, scale=1.0):
        a = lax.broadcasted_iota(jnp.int32, (chunk, chunk), 0) // head
        b = lax.broadcasted_iota(jnp.int32, (chunk, chunk), 1) // head
        return jnp.where(a == b, scale, 0.0).astype(dtype)

    def head_sums(x, block, precision=None):
        return jnp.concatenate(
            [
                jnp.dot(
                    x[:, c : c + chunk], block, preferred_element_type=f32, precision=precision
                )
                for c in range(0, inner, chunk)
            ],
            axis=1,
        )

    @pl.when(step == 0)
    def _():
        copy.start()
        for m in range(3):
            for j in range(count):
                vec_ref[m, :, j * width : (j + 1) * width] = joined_ref[
                    j, :, m * width : (m + 1) * width
                ].astype(f32)
        keys = vec_ref[1]
        unit = keys * lax.rsqrt(
            head_sums(keys * keys, ones(f32), lax.Precision.HIGHEST) + norm_eps
        )
        vec_ref[3] = unit
        vec_ref[4] = unit * removal_ref[...]

    lane = lax.broadcasted_iota(jnp.int32, (values, inner), 1) % head
    row = lax.broadcasted_iota(jnp.int32, (values, inner), 0)
    diagonal = lane == row

    def vector(m, b):
        return vec_ref[m, pl.ds(step * batch + b, 1), :]

    def block_sums(tables):
        cut = [t[:, c : c + chunk] for t in tables for c in range(0, inner, chunk)]
        sums = jnp.dot(jnp.concatenate(cut, axis=0), ones(bf16), preferred_element_type=f32)
        pieces = [sums[k * values : (k + 1) * values] for k in range(len(cut))]
        per = inner // chunk
        return [
            jnp.concatenate(pieces[k * per : (k + 1) * per], axis=1) for k in range(len(tables))
        ]

    recalled = block_sums([(state_ref[b] * vector(3, b)).astype(bf16) for b in range(batch)])
    spread = block_sums(
        [jnp.where(diagonal, vector(2, b), 0.0).astype(bf16) for b in range(batch)]
    )
    for b in range(batch):
        decay = decay_ref[pl.ds(step * batch + b, 1), :]
        state_out_ref[b] = (
            state_ref[b] * decay - recalled[b] * vector(4, b) + spread[b] * vector(1, b)
        )
    read = block_sums([(state_out_ref[b] * vector(0, b)).astype(bf16) for b in range(batch)])
    for b in range(batch):
        readout_ref[pl.ds(step * batch + b, 1), :] = jnp.sum(
            jnp.where(diagonal, read[b], 0.0), axis=0, keepdims=True
        )

    @pl.when(step == steps - 1)
    def _():
        readout = readout_ref[...]
        mean_block = ones(f32, 1.0 / head)
        center = readout - head_sums(readout, mean_block, lax.Precision.HIGHEST)
        variance = head_sums(center * center, mean_block, lax.Precision.HIGHEST)
        grouped = (center * lax.rsqrt(variance + group_eps) * gain_ref[...]).astype(bf16)
        copy.wait()
        residual = hidden_ref[...].astype(f32) + jnp.dot(
            grouped, w_out_buf[...], preferred_element_type=f32
        )
        residual_ref[...] = residual
        expert_ref[...] = scaled_rows(residual, ffn_gain_ref[...]).astype(bf16)


def mixer(state_in, joined, decay, removal, group_gain, hidden_in, ffn_gain, w_out):
    seqs, head, inner = state_in.shape
    width = hidden_in.shape[1]
    batch = 4 if seqs % 4 == 0 else 1

    def whole(shape):
        return pl.BlockSpec(shape, lambda i: (0,) * len(shape))

    by_seq = pl.BlockSpec((batch, head, inner), lambda i: (i, 0, 0))
    return pl.pallas_call(
        functools.partial(mixer_kernel, head=head),
        grid=(seqs // batch,),
        out_shape=(
            jax.ShapeDtypeStruct(state_in.shape, f32),
            jax.ShapeDtypeStruct((seqs, width), f32),
            jax.ShapeDtypeStruct((seqs, width), bf16),
        ),
        in_specs=[
            by_seq,
            whole(joined.shape),
            whole((seqs, inner)),
            whole((seqs, inner)),
            whole((1, inner)),
            whole((seqs, width)),
            whole((1, width)),
            ANY,
        ],
        out_specs=(by_seq, whole((seqs, width)), whole((seqs, width))),
        scratch_shapes=[
            pltpu.VMEM((5, seqs, inner), f32),
            pltpu.VMEM((seqs, inner), f32),
            pltpu.VMEM(w_out.shape, bf16),
            pltpu.SemaphoreType.DMA(()),
        ],
        compiler_params=pltpu.CompilerParams(vmem_limit_bytes=32 * 2**20),
        name="mixer",
    )(
        state_in, joined, decay, removal, group_gain.reshape(1, -1), hidden_in,
        ffn_gain.reshape(1, -1), w_out,
    )


def expert_kernel(*refs, count):
    pieces = refs[:count]
    gate_ref, up_ref, down_ref = refs[count : count + 3]
    outs = refs[count + 3 : -5]
    gate_buf, up_buf, down_buf, hidden_ref, sems = refs[-5:]
    rows = pieces[0].shape[0]
    units = gate_buf.shape[0]
    cuts = 2
    part = units // cuts
    copies = []
    for c in range(cuts):
        span = pl.ds(c * part, part)
        for m, (source, target) in enumerate(((gate_ref, gate_buf), (up_ref, up_buf))):
            copies.append(
                pltpu.make_async_copy(source.at[span], target.at[span], sems.at[2 * c + m])
            )
    last = pltpu.make_async_copy(down_ref, down_buf, sems.at[2 * cuts])
    for copy in copies:
        copy.start()
    last.start()
    tokens = jnp.concatenate([piece[...] for piece in pieces], axis=0)
    for c in range(cuts):
        span = pl.ds(c * part, part)
        copies[2 * c].wait()
        gate = lax.dot_general(tokens, gate_buf[span], NT, preferred_element_type=f32)
        copies[2 * c + 1].wait()
        up = lax.dot_general(tokens, up_buf[span], NT, preferred_element_type=f32)
        hidden_ref[:, c * part : (c + 1) * part] = (jax.nn.silu(gate) * up).astype(bf16)
    last.wait()
    result = jnp.dot(hidden_ref[...], down_buf[...], preferred_element_type=f32).astype(bf16)
    for d in range(count):
        outs[2 * (d // 4) + d % 2][d % 4 // 2] = result[d * rows : (d + 1) * rows]


def run_experts(pieces, w_gate, w_up, w_down):
    count = len(pieces)
    rows, width = pieces[0].shape
    units = w_down.shape[0]
    return pl.pallas_call(
        functools.partial(expert_kernel, count=count),
        out_shape=[jax.ShapeDtypeStruct((2, rows, width), bf16)] * (count // 2),
        in_specs=[VM] * count + [ANY] * 3,
        out_specs=[VM] * (count // 2),
        scratch_shapes=[pltpu.VMEM((units, width), bf16)] * 3
        + [pltpu.VMEM((count * rows, units), bf16), pltpu.SemaphoreType.DMA((5,))],
        compiler_params=pltpu.CompilerParams(vmem_limit_bytes=24 * 2**20),
        name="experts",
    )(*pieces, w_gate.T, w_up.T, w_down)


def add(a, b):
    return (a.astype(f32) + b.astype(f32)).astype(bf16)


def shards(
    hidden_in,
    state_in,
    norm_gain,
    w_recept,
    w_key,
    w_value,
    decay_base,
    w_decay_down,
    w_decay_up,
    w_remove_down,
    w_remove_up,
    group_gain,
    w_out,
    ffn_gain,
    routes,
    route_gate,
    w_gate,
    w_up,
    w_down,
):
    place = lax.axis_index("ep")
    groups = lax.axis_size("ep") // EXP_SPLIT
    normed = norm_rows(hidden_in, norm_gain)
    pieces = gather_pieces(hidden_in)
    spread = project(pieces, (w_recept, w_key, w_value), norm_gain)
    joined = lax.all_to_all(spread, "ep", split_axis=0, concat_axis=0, tiled=True)
    decay_rate = decay_of(normed, w_decay_down, w_decay_up, decay_base)
    removal = removal_of(normed, w_remove_down, w_remove_up)
    state_out, residual, expert_in = mixer(
        state_in, joined, decay_rate, removal, group_gain, hidden_in, ffn_gain, w_out
    )
    outs = run_experts(gather_pieces(expert_in), w_gate, w_up, w_down)
    mixed = residual
    for d in range(groups - 1, -1, -1):
        by_side = add(outs[2 * d], swap(outs[2 * d + 1], 1))
        part = add(by_side[0], swap(by_side[1], 2))
        if d:
            part = swap(part, EXP_SPLIT * d)
        weight = jnp.sum(
            jnp.where(routes == (place // EXP_SPLIT) ^ d, route_gate, 0.0), axis=1, keepdims=True
        )
        mixed = mixed + weight * part.astype(f32)
    return (mixed.astype(bf16), state_out)


def solution(mesh):
    placed = (
        P(("grp", "ep"), None),
        P(("grp", "ep"), None, None),
        P(),
        P(None, "ep"),
        P(None, "ep"),
        P(None, "ep"),
        P(),
        P(),
        P(),
        P(),
        P(),
        P(),
        P(),
        P(),
        P(("grp", "ep"), None),
        P(("grp", "ep"), None),
        P(None, "ep"),
        P(None, "ep"),
        P("ep", None),
    )
    return jax.shard_map(
        shards,
        mesh=mesh,
        in_specs=placed,
        out_specs=(P(("grp", "ep"), None), P(("grp", "ep"), None, None)),
        check_vma=False,
    )
```

```python
import functools

import jax
import jax.numpy as jnp
from jax import lax
from jax.experimental import pallas as pl
from jax.experimental.pallas import tpu as pltpu
from jax.sharding import PartitionSpec as P

EXP_SPLIT = 4

norm_eps = 1e-06
group_eps = 0.00064
f32 = jnp.float32
bf16 = jnp.bfloat16
NT = (((1,), (1,)), ((), ()))
VM = pl.BlockSpec(memory_space=pltpu.VMEM)
ANY = pl.BlockSpec(memory_space=pl.ANY)


def scaled_rows(values, scale_gain):
    floats = values.astype(f32)
    return (
        floats
        * lax.rsqrt(jnp.mean(floats * floats, axis=-1, keepdims=True) + norm_eps)
        * scale_gain
    )


def decay_of(normed, w_decay_down, w_decay_up, decay_base):
    decay_low = jnp.dot(normed, w_decay_down, preferred_element_type=f32).astype(bf16)
    decay_act = jnp.tanh(decay_low.astype(f32)).astype(bf16)
    decay_pre = decay_base + jnp.dot(decay_act, w_decay_up, preferred_element_type=f32)
    return jnp.exp(-jnp.exp(-jax.nn.softplus(-decay_pre) - 0.5))


def removal_of(normed, w_remove_down, w_remove_up):
    remove_low = jnp.dot(normed, w_remove_down, preferred_element_type=f32).astype(bf16)
    return jax.nn.sigmoid(jnp.dot(remove_low, w_remove_up, preferred_element_type=f32))


def in_hbm(array):
    return pltpu.with_memory_space_constraint(array, pltpu.HBM)


def swap(piece, bits):
    size = lax.axis_size("ep")
    return lax.ppermute(piece, "ep", [(i, i ^ bits) for i in range(size)])


def gather_pieces(own):
    size = lax.axis_size("ep")
    pieces = {0: own}
    for d in range(size // 4 - 1, 0, -1):
        pieces[4 * d] = swap(own, 4 * d)
    for d in list(pieces):
        pieces[d + 2] = swap(pieces[d], 2)
    for d in list(pieces):
        pieces[d + 1] = swap(pieces[d], 1)
    return [pieces[d] for d in range(size)]


def norm_kernel(x_ref, gain_ref, out_ref):
    out_ref[...] = scaled_rows(x_ref[...], gain_ref[...]).astype(bf16)


def norm_rows(values, gain):
    return pl.pallas_call(
        norm_kernel,
        out_shape=jax.ShapeDtypeStruct(values.shape, bf16),
        in_specs=[VM, VM],
        out_specs=VM,
        name="norm_rows",
    )(values, gain.reshape(1, -1))


def project_kernel(place_ref, *refs):
    out_ref = refs[-1]
    count = out_ref.shape[0]
    pieces, weights = refs[:count], refs[count : count + 3]
    rows = pieces[0].shape[0]
    width = weights[0].shape[0]
    gain = refs[count + 3][...]
    tokens = jnp.concatenate(
        [scaled_rows(piece[...], gain).astype(bf16) for piece in pieces], axis=0
    )
    parts = [
        lax.dot_general(tokens, w[...], NT, preferred_element_type=f32).astype(bf16)
        for w in weights
    ]
    place = place_ref[0]
    for d in range(count):
        target = place ^ d
        for m in range(3):
            out_ref[target, :, m * width : (m + 1) * width] = parts[m][d * rows : (d + 1) * rows]


def project(pieces, weights, gain):
    count = len(pieces)
    rows = pieces[0].shape[0]
    width = weights[0].shape[1]
    return pl.pallas_call(
        project_kernel,
        out_shape=jax.ShapeDtypeStruct((count, rows, 3 * width), bf16),
        in_specs=[pl.BlockSpec(memory_space=pltpu.SMEM)] + [VM] * (count + 4),
        out_specs=VM,
        compiler_params=pltpu.CompilerParams(vmem_limit_bytes=16 * 2**20),
        name="project",
    )(lax.axis_index("ep").astype(jnp.int32).reshape(1), in_hbm(pieces[0]), *pieces[1:], *[in_hbm(w.T) for w in weights], in_hbm(gain.reshape(1, -1)))


def mixer_kernel(
    state_ref, joined_ref, decay_ref, removal_ref, gain_ref, hidden_ref, ffn_gain_ref, w_out_ref,
    state_out_ref, residual_ref, expert_ref,
    vec_ref, readout_ref, w_out_buf, sem, *, head,
):
    step = pl.program_id(0)
    steps = pl.num_programs(0)
    batch, values, inner = state_ref.shape
    chunk = min(256, inner)
    count = joined_ref.shape[0]
    width = inner // count
    copy = pltpu.make_async_copy(w_out_ref, w_out_buf, sem)

    def ones(dtype, scale=1.0):
        a = lax.broadcasted_iota(jnp.int32, (chunk, chunk), 0) // head
        b = lax.broadcasted_iota(jnp.int32, (chunk, chunk), 1) // head
        return jnp.where(a == b, scale, 0.0).astype(dtype)

    def head_sums(x, block, precision=None):
        return jnp.concatenate(
            [
                jnp.dot(
                    x[:, c : c + chunk], block, preferred_element_type=f32, precision=precision
                )
                for c in range(0, inner, chunk)
            ],
            axis=1,
        )

    @pl.when(step == 0)
    def _():
        copy.start()
        for m in range(3):
            for j in range(count):
                vec_ref[m, :, j * width : (j + 1) * width] = joined_ref[
                    j, :, m * width : (m + 1) * width
                ].astype(f32)
        keys = vec_ref[1]
        unit = keys * lax.rsqrt(
            head_sums(keys * keys, ones(f32), lax.Precision.HIGHEST) + norm_eps
        )
        vec_ref[3] = unit
        vec_ref[4] = unit * removal_ref[...]

    lane = lax.broadcasted_iota(jnp.int32, (values, inner), 1) % head
    row = lax.broadcasted_iota(jnp.int32, (values, inner), 0)
    diagonal = lane == row

    def vector(m, b):
        return vec_ref[m, pl.ds(step * batch + b, 1), :]

    def block_sums(tables):
        cut = [t[:, c : c + chunk] for t in tables for c in range(0, inner, chunk)]
        sums = jnp.dot(jnp.concatenate(cut, axis=0), ones(bf16), preferred_element_type=f32)
        pieces = [sums[k * values : (k + 1) * values] for k in range(len(cut))]
        per = inner // chunk
        return [
            jnp.concatenate(pieces[k * per : (k + 1) * per], axis=1) for k in range(len(tables))
        ]

    recalled = block_sums([(state_ref[b] * vector(3, b)).astype(bf16) for b in range(batch)])
    spread = block_sums(
        [jnp.where(diagonal, vector(2, b), 0.0).astype(bf16) for b in range(batch)]
    )
    for b in range(batch):
        decay = decay_ref[pl.ds(step * batch + b, 1), :]
        state_out_ref[b] = (
            state_ref[b] * decay - recalled[b] * vector(4, b) + spread[b] * vector(1, b)
        )
    read = block_sums([(state_out_ref[b] * vector(0, b)).astype(bf16) for b in range(batch)])
    for b in range(batch):
        readout_ref[pl.ds(step * batch + b, 1), :] = jnp.sum(
            jnp.where(diagonal, read[b], 0.0), axis=0, keepdims=True
        )

    @pl.when(step == steps - 1)
    def _():
        readout = readout_ref[...]
        mean_block = ones(f32, 1.0 / head)
        center = readout - head_sums(readout, mean_block, lax.Precision.HIGHEST)
        variance = head_sums(center * center, mean_block, lax.Precision.HIGHEST)
        grouped = (center * lax.rsqrt(variance + group_eps) * gain_ref[...]).astype(bf16)
        copy.wait()
        residual = hidden_ref[...].astype(f32) + jnp.dot(
            grouped, w_out_buf[...], preferred_element_type=f32
        )
        residual_ref[...] = residual
        expert_ref[...] = scaled_rows(residual, ffn_gain_ref[...]).astype(bf16)


def mixer(state_in, joined, decay, removal, group_gain, hidden_in, ffn_gain, w_out):
    seqs, head, inner = state_in.shape
    width = hidden_in.shape[1]
    batch = 4 if seqs % 4 == 0 else 1

    def whole(shape):
        return pl.BlockSpec(shape, lambda i: (0,) * len(shape))

    by_seq = pl.BlockSpec((batch, head, inner), lambda i: (i, 0, 0))
    return pl.pallas_call(
        functools.partial(mixer_kernel, head=head),
        grid=(seqs // batch,),
        out_shape=(
            jax.ShapeDtypeStruct(state_in.shape, f32),
            jax.ShapeDtypeStruct((seqs, width), f32),
            jax.ShapeDtypeStruct((seqs, width), bf16),
        ),
        in_specs=[
            by_seq,
            whole(joined.shape),
            whole((seqs, inner)),
            whole((seqs, inner)),
            whole((1, inner)),
            whole((seqs, width)),
            whole((1, width)),
            ANY,
        ],
        out_specs=(by_seq, whole((seqs, width)), whole((seqs, width))),
        scratch_shapes=[
            pltpu.VMEM((5, seqs, inner), f32),
            pltpu.VMEM((seqs, inner), f32),
            pltpu.VMEM(w_out.shape, bf16),
            pltpu.SemaphoreType.DMA(()),
        ],
        compiler_params=pltpu.CompilerParams(vmem_limit_bytes=32 * 2**20),
        name="mixer",
    )(
        in_hbm(state_in), joined, decay, removal, group_gain.reshape(1, -1), hidden_in,
        ffn_gain.reshape(1, -1), in_hbm(w_out),
    )


def expert_kernel(*refs, count):
    pieces = refs[:count]
    gate_ref, up_ref, down_ref = refs[count : count + 3]
    outs = refs[count + 3 : -5]
    gate_buf, up_buf, down_buf, hidden_ref, sems = refs[-5:]
    rows = pieces[0].shape[0]
    units = gate_buf.shape[0]
    cuts = 2
    part = units // cuts
    copies = []
    for c in range(cuts):
        span = pl.ds(c * part, part)
        for m, (source, target) in enumerate(((gate_ref, gate_buf), (up_ref, up_buf))):
            copies.append(
                pltpu.make_async_copy(source.at[span], target.at[span], sems.at[2 * c + m])
            )
    last = pltpu.make_async_copy(down_ref, down_buf, sems.at[2 * cuts])
    for copy in copies:
        copy.start()
    last.start()
    tokens = jnp.concatenate([piece[...] for piece in pieces], axis=0)
    for c in range(cuts):
        span = pl.ds(c * part, part)
        copies[2 * c].wait()
        gate = lax.dot_general(tokens, gate_buf[span], NT, preferred_element_type=f32)
        copies[2 * c + 1].wait()
        up = lax.dot_general(tokens, up_buf[span], NT, preferred_element_type=f32)
        hidden_ref[:, c * part : (c + 1) * part] = (jax.nn.silu(gate) * up).astype(bf16)
    last.wait()
    result = jnp.dot(hidden_ref[...], down_buf[...], preferred_element_type=f32).astype(bf16)
    for d in range(count):
        outs[2 * (d // 4) + d % 2][d % 4 // 2] = result[d * rows : (d + 1) * rows]


def run_experts(pieces, w_gate, w_up, w_down):
    count = len(pieces)
    rows, width = pieces[0].shape
    units = w_down.shape[0]
    return pl.pallas_call(
        functools.partial(expert_kernel, count=count),
        out_shape=[jax.ShapeDtypeStruct((2, rows, width), bf16)] * (count // 2),
        in_specs=[VM] * count + [ANY] * 3,
        out_specs=[VM] * (count // 2),
        scratch_shapes=[pltpu.VMEM((units, width), bf16)] * 3
        + [pltpu.VMEM((count * rows, units), bf16), pltpu.SemaphoreType.DMA((5,))],
        compiler_params=pltpu.CompilerParams(vmem_limit_bytes=24 * 2**20),
        name="experts",
    )(*pieces, w_gate.T, w_up.T, w_down)


def add(a, b):
    return (a.astype(f32) + b.astype(f32)).astype(bf16)


def shards(
    hidden_in,
    state_in,
    norm_gain,
    w_recept,
    w_key,
    w_value,
    decay_base,
    w_decay_down,
    w_decay_up,
    w_remove_down,
    w_remove_up,
    group_gain,
    w_out,
    ffn_gain,
    routes,
    route_gate,
    w_gate,
    w_up,
    w_down,
):
    place = lax.axis_index("ep")
    groups = lax.axis_size("ep") // EXP_SPLIT
    normed = norm_rows(hidden_in, norm_gain)
    pieces = gather_pieces(hidden_in)
    spread = project(pieces, (w_recept, w_key, w_value), norm_gain)
    joined = lax.all_to_all(spread, "ep", split_axis=0, concat_axis=0, tiled=True)
    decay_rate = decay_of(normed, w_decay_down, w_decay_up, decay_base)
    removal = removal_of(normed, w_remove_down, w_remove_up)
    state_out, residual, expert_in = mixer(
        state_in, joined, decay_rate, removal, group_gain, hidden_in, ffn_gain, w_out
    )
    outs = run_experts(gather_pieces(expert_in), w_gate, w_up, w_down)
    mixed = residual
    for d in range(groups - 1, -1, -1):
        by_side = add(outs[2 * d], swap(outs[2 * d + 1], 1))
        part = add(by_side[0], swap(by_side[1], 2))
        if d:
            part = swap(part, EXP_SPLIT * d)
        weight = jnp.sum(
            jnp.where(routes == (place // EXP_SPLIT) ^ d, route_gate, 0.0), axis=1, keepdims=True
        )
        mixed = mixed + weight * part.astype(f32)
    return (mixed.astype(bf16), state_out)


def solution(mesh):
    placed = (
        P(("grp", "ep"), None),
        P(("grp", "ep"), None, None),
        P(),
        P(None, "ep"),
        P(None, "ep"),
        P(None, "ep"),
        P(),
        P(),
        P(),
        P(),
        P(),
        P(),
        P(),
        P(),
        P(("grp", "ep"), None),
        P(("grp", "ep"), None),
        P(None, "ep"),
        P(None, "ep"),
        P("ep", None),
    )
    return jax.shard_map(
        shards,
        mesh=mesh,
        in_specs=placed,
        out_specs=(P(("grp", "ep"), None), P(("grp", "ep"), None, None)),
        check_vma=False,
    )
```
